32 devices in a mesh: dp: 4 (over y, x), kv: 4 (over z), tp: 2 (over core).
Axes of the slice: x: 2, y: 2, z: 4, core: 2. Of those that a mesh axis runs over, the one named last changes fastest.
Arguments:
- tokens: bfloat16 [32, 4096], P('dp', ('kv', 'tp')), as said below
- query_weight: bfloat16 [4096, 16, 128], P(None, 'tp', 'kv'), may hold values from -0.09375 to 0.09375
- key_weight: bfloat16 [4096, 16, 128], P(None, 'tp', 'kv'), may hold values from -0.09375 to 0.09375
- value_weight: bfloat16 [4096, 16, 256], P(None, 'tp', 'kv'), may hold values from -0.09375 to 0.09375
- gate_weight: bfloat16 [4096, 16, 256], P(None, 'tp', 'kv'), may hold values from -0.09375 to 0.09375
- decay_weight: bfloat16 [4096, 16, 128], P(None, 'tp', 'kv'), may hold values from -0.09375 to 0.09375
- decay_bias: float32 [16, 128], P('tp'), may hold values from -8 to 2
- states: float32 [32, 16, 128, 256], P(('dp', 'kv'), 'tp'), may hold values from -4 to 4
- head_gain: float32 [16, 256], P('tp'), may hold values from 0.1 to 1.9
- out_weight: bfloat16 [4096, 4096], P(None, ('kv', 'tp')), as said below
- norm1_gain: float32 [4096], P(('kv', 'tp')), may hold values from 0.1 to 1.9
- norm1_bias: float32 [4096], P(('kv', 'tp')), may hold values from -3 to 3
- up_weight: bfloat16 [4096, 16384], P(None, ('kv', 'tp')), may hold values from -0.09375 to 0.09375
- down_weight: bfloat16 [16384, 4096], P(('kv', 'tp')), as said below
- norm2_gain: float32 [4096], P(('kv', 'tp')), may hold values from 0.1 to 1.9
- norm2_bias: float32 [4096], P(('kv', 'tp')), may hold values from -3 to 3
Outputs:
- layer_out: bfloat16 [32, 4096], P('dp', ('kv', 'tp'))
- new_states: float32 [32, 16, 128, 256], P(('dp', 'kv'), 'tp')
The draws below stay inside these ranges and needn't reach their ends.
Inputs may be any that keep to these rules, and one draw needn't show every extreme that they name: `tokens`: each block of 64 features has its own scale. `out_weight`: entries lie within 13 / sqrt(4096) of zero. `down_weight`: entries lie within 14 / sqrt(16384) of zero.
All inputs are finite; a program needn't handle non-finite values.
Results may differ from the reference program's by a relative error of at most 0.009.
Values may be sent and summed in bfloat16 or wider, within the bound.
A program may use at most 128 MiB of HBM per device.

```python
import jax
import jax.numpy as jnp
from jax import lax

D = 4096
HEADS = 16
KEY_DIM = 128
VALUE_DIM = 256
MIXER_UNITS = 16384
ROWS = 32


def draw_tokens(key, part):
    base_key, scale_key = jax.random.split(key, 2)
    column_scale = jnp.exp(jax.random.uniform(scale_key, (D // 64,), jnp.float32, -1.0, 1.0))
    column_scale = jnp.repeat(column_scale, 64)
    values = jax.random.normal(base_key, (ROWS, D), jnp.float32)
    return (values * column_scale).astype(jnp.bfloat16)


def draw_out_weight(key, part):
    noise_key, left_key, right_key = jax.random.split(jax.random.fold_in(key, 31), 3)
    fan_in = HEADS * VALUE_DIM
    left = jnp.clip(jax.random.normal(left_key, (fan_in, 1), jnp.float32), -3.0, 3.0)
    right = jnp.clip(jax.random.normal(right_key, (1, D), jnp.float32), -3.0, 3.0)
    noise = jnp.clip(jax.random.normal(noise_key, (fan_in, D), jnp.float32), -6.0, 6.0)
    common = 0.8 * left * right
    return ((0.6 * noise + common) * fan_in ** (-0.5)).astype(jnp.bfloat16)


def draw_down_weight(key, part):
    noise_key, offset_key = jax.random.split(jax.random.fold_in(key, 47), 2)
    noise = jnp.clip(jax.random.normal(noise_key, (MIXER_UNITS, D), jnp.float32), -6.0, 6.0)
    offset = jax.random.uniform(offset_key, (1, D), jnp.float32, -5.0, 5.0)
    values = noise * MIXER_UNITS ** (-0.5) + offset / MIXER_UNITS
    return values.astype(jnp.bfloat16)


def block_levels(own_key, dims, shards, low, top_value):
    level, own = 1.0, jax.random.fold_in(own_key, 6)
    for dim, blocks in shards:
        steps = jnp.exp(jax.random.uniform(jax.random.fold_in(own, dim), (blocks,), jnp.float32, low / len(shards), top_value / len(shards)))
        level = level * jnp.repeat(steps, dims[dim] // blocks).reshape([-1 if axis == dim else 1 for axis in range(len(dims))])
    return level


def scatter_about(stream_key, shape, scale, reach, cuts=(), kind=jnp.bfloat16):
    values = scale * jax.random.normal(stream_key, shape, jnp.float32)
    if cuts:
        values = values * block_levels(stream_key, shape, cuts, -0.22, 0.18)
    return jnp.clip(values, -reach, reach).astype(kind)


def setup_inputs(seed: int = 0) -> dict:
    keys = jax.random.split(jax.random.key(seed), 17)
    return {
        "tokens": draw_tokens(jax.random.fold_in(keys[16], 71), 0),
        "query_weight": scatter_about(keys[1], (D, HEADS, KEY_DIM), D ** -0.5, 0.09375, ((1, 2), (2, 4))),
        "key_weight": scatter_about(keys[2], (D, HEADS, KEY_DIM), D ** -0.5, 0.09375, ((1, 2), (2, 4))),
        "value_weight": scatter_about(keys[3], (D, HEADS, VALUE_DIM), D ** -0.5, 0.09375, ((1, 2), (2, 4))),
        "gate_weight": scatter_about(keys[4], (D, HEADS, VALUE_DIM), D ** -0.5, 0.09375, ((1, 2), (2, 4))),
        "decay_weight": scatter_about(keys[5], (D, HEADS, KEY_DIM), D ** -0.5, 0.09375, ((1, 2), (2, 4))),
        "decay_bias": jnp.clip(-8.0 + 10.0 * jax.random.uniform(keys[6], (HEADS, KEY_DIM), jnp.float32) ** block_levels(keys[6], (HEADS, KEY_DIM), ((0, 2),), -0.2, 0.2), -8.0, 2.0),
        "states": scatter_about(keys[7], (ROWS, HEADS, KEY_DIM, VALUE_DIM), 0.5, 4.0, ((0, 16), (1, 2)), jnp.float32),
        "head_gain": jnp.clip(1.0 + 0.18 * jax.random.normal(keys[8], (HEADS, VALUE_DIM), jnp.float32), 0.1, 1.9),
        "out_weight": draw_out_weight(jax.random.fold_in(keys[16], 71), 0),
        "norm1_gain": jnp.clip(1.0 + 0.18 * jax.random.normal(keys[10], (D,), jnp.float32), 0.1, 1.9),
        "norm1_bias": scatter_about(keys[11], (D,), 0.5, 3.0, ((0, 8),), jnp.float32),
        "up_weight": scatter_about(keys[12], (D, MIXER_UNITS), D ** -0.5, 0.09375, ((1, 8),)),
        "down_weight": draw_down_weight(jax.random.fold_in(keys[16], 71), 0),
        "norm2_gain": jnp.clip(1.0 + 0.18 * jax.random.normal(keys[14], (D,), jnp.float32), 0.1, 1.9),
        "norm2_bias": scatter_about(keys[15], (D,), 0.5, 3.0, ((0, 8),), jnp.float32),
    }


ALPHA = 2.0 ** 0.5
TAU = 16.0
LN_EPS = 1e-05
RMS_EPS = 1e-06

def project(inputs, weight):
    flattened = weight.reshape(weight.shape[0], -1)
    return jnp.dot(inputs, flattened, preferred_element_type=jnp.float32).astype(jnp.bfloat16)

def normalize(inputs, row_gain, row_shift):
    average = lax.optimization_barrier(jnp.sum(inputs, axis=-1, keepdims=True)) / inputs.shape[-1]
    spread = lax.optimization_barrier(jnp.sum(inputs * inputs, axis=-1, keepdims=True)) / inputs.shape[-1] - average * average
    return ((inputs - average) * lax.rsqrt(spread + LN_EPS) * row_gain + row_shift).astype(jnp.bfloat16)

def reference(tokens, query_weight, key_weight, value_weight, gate_weight, decay_weight, decay_bias, states, head_gain, out_weight, norm1_gain, norm1_bias, up_weight, down_weight, norm2_gain, norm2_bias):
    row_count = tokens.shape[0]
    query_rows = project(tokens, query_weight).astype(jnp.float32).reshape(row_count, HEADS, KEY_DIM) * KEY_DIM ** (-0.5)
    key_rows = project(tokens, key_weight).astype(jnp.float32).reshape(row_count, HEADS, KEY_DIM)
    decay_rows = project(tokens, decay_weight).astype(jnp.float32).reshape(row_count, HEADS, KEY_DIM)
    value_rows = project(tokens, value_weight).astype(jnp.float32).reshape(row_count, HEADS, VALUE_DIM)
    gate_rows = project(tokens, gate_weight).astype(jnp.float32).reshape(row_count, HEADS, VALUE_DIM)
    retain = jnp.exp(jax.nn.log_sigmoid(decay_rows + decay_bias) / TAU)
    new_states = retain[..., None] * states + key_rows[..., :, None] * value_rows[..., None, :]
    readout = jnp.einsum('rhk,rhkv->rhv', query_rows, new_states, precision=lax.Precision.HIGHEST)
    readout = readout * lax.rsqrt(lax.optimization_barrier(jnp.mean(readout * readout, axis=-1, keepdims=True)) + RMS_EPS) * head_gain
    attended = (readout * jax.nn.silu(gate_rows)).astype(jnp.bfloat16).reshape(row_count, HEADS * VALUE_DIM)
    mixed_heads = jnp.dot(attended, out_weight, preferred_element_type=jnp.float32)
    residual_one = ALPHA * tokens.astype(jnp.float32) + mixed_heads
    normed = normalize(residual_one, norm1_gain, norm1_bias)
    lifted = jnp.dot(normed, up_weight, preferred_element_type=jnp.float32)
    hidden = jnp.square(jax.nn.relu(lifted)).astype(jnp.bfloat16)
    residual_two = ALPHA * normed.astype(jnp.float32) + jnp.dot(hidden, down_weight, preferred_element_type=jnp.float32)
    return (normalize(residual_two, norm2_gain, norm2_bias), new_states)
```

```python
import functools

import jax
import jax.numpy as jnp
from jax import lax
from jax.experimental import pallas as pl
from jax.experimental.pallas import tpu as pltpu
from jax.sharding import PartitionSpec as P

D = 4096
KEY_DIM = 128


ALPHA = 2.0**0.5
TAU = 16.0
LN_EPS = 1e-05
RMS_EPS = 1e-06


def project_flat(inputs, weight):
    flattened = weight.reshape(weight.shape[0], -1)
    return jnp.dot(inputs, flattened, preferred_element_type=jnp.float32).astype(jnp.bfloat16)


def normalize(inputs, average, spread, row_gain, row_shift):
    return ((inputs - average) * lax.rsqrt(spread + LN_EPS) * row_gain + row_shift).astype(
        jnp.bfloat16
    )


def body(
    tokens,
    query_weight,
    key_weight,
    value_weight,
    gate_weight,
    decay_weight,
    decay_bias,
    states,
    head_gain,
    out_weight,
    norm1_gain,
    norm1_bias,
    up_weight,
    down_weight,
    norm2_gain,
    norm2_bias,
):
    whole = lax.all_gather(tokens, ("kv", "tp"), axis=1, tiled=True)
    weights_list = (query_weight, key_weight, decay_weight, value_weight, gate_weight)
    packed = jnp.concatenate([project_flat(whole, weight) for weight in weights_list], axis=1)
    arrived = lax.all_to_all(packed, "kv", split_axis=0, concat_axis=0, tiled=True)
    groups = lax.axis_size("kv")
    seq_count = whole.shape[0] // groups
    local_heads = query_weight.shape[1]
    unpacked = []
    start = 0
    for weight in weights_list:
        channels = weight.shape[2]
        width = local_heads * channels
        block = arrived[:, start : start + width].reshape(groups, seq_count, local_heads, channels)
        block = block.transpose(1, 2, 0, 3).reshape(seq_count, local_heads, groups * channels)
        unpacked.append(block.astype(jnp.float32))
        start = start + width
    query_rows = unpacked[0] * KEY_DIM ** (-0.5)
    key_rows = unpacked[1]
    decay_rows = unpacked[2]
    value_rows = unpacked[3]
    gate_rows = unpacked[4]
    retain = jnp.exp(jax.nn.log_sigmoid(decay_rows + decay_bias) / TAU)
    new_states = retain[..., None] * states + key_rows[..., :, None] * value_rows[..., None, :]
    readout = jnp.einsum("shk,shkv->shv", query_rows, new_states, precision=lax.Precision.HIGHEST)
    readout = (
        readout
        * lax.rsqrt(jnp.mean(readout * readout, axis=-1, keepdims=True) + RMS_EPS)
        * head_gain
    )
    attended = (readout * jax.nn.silu(gate_rows)).astype(jnp.bfloat16)
    seq_count, local_heads, value_width = attended.shape
    flat_width = local_heads * value_width
    collected = lax.all_gather(
        attended.reshape(1, seq_count, flat_width), ("kv", "tp"), axis=0, tiled=True
    )
    halves = lax.axis_size("tp")
    collected = collected.reshape(-1, halves, seq_count, flat_width)
    columns = out_weight.shape[1]
    out_parts = out_weight.reshape(halves, flat_width, columns)
    mixed_heads = jnp.einsum(
        "atsc,tcd->asd", collected, out_parts, preferred_element_type=jnp.float32
    ).reshape(-1, columns)
    residual_one = ALPHA * tokens.astype(jnp.float32) + mixed_heads
    offset = lax.axis_index(("kv", "tp")) * columns
    totals = lax.psum(
        (
            jnp.sum(residual_one, axis=-1, keepdims=True),
            jnp.sum(residual_one * residual_one, axis=-1, keepdims=True),
        ),
        ("kv", "tp"),
    )
    average = totals[0] / D
    spread = totals[1] / D - average * average
    normed_own = normalize(residual_one, average, spread, norm1_gain, norm1_bias)
    normed = lax.all_gather(normed_own, ("kv", "tp"), axis=1, tiled=True)
    lifted = jnp.dot(normed, up_weight, preferred_element_type=jnp.float32)
    hidden = jnp.square(jax.nn.relu(lifted)).astype(jnp.bfloat16)
    mixer_term = jnp.dot(hidden, down_weight, preferred_element_type=jnp.float32)
    mixer_all = lax.psum(mixer_term, ("kv", "tp"))
    residual_two = ALPHA * normed.astype(jnp.float32) + mixer_all
    average = jnp.sum(residual_two, axis=-1, keepdims=True) / D
    spread = jnp.sum(residual_two * residual_two, axis=-1, keepdims=True) / D - average * average
    own_rows = lax.dynamic_slice_in_dim(residual_two, offset, columns, 1)
    layer_out = normalize(own_rows, average, spread, norm2_gain, norm2_bias)
    return (layer_out, new_states)


MESH = pl.DeviceIdType.MESH
F32 = jnp.float32
BF16 = jnp.bfloat16


def dot_nt(left, right):
    return lax.dot_general(left, right, (((1,), (1,)), ((), ())), preferred_element_type=F32)


def layer_kernel(
    groups, halves, tokens, wq, wk, wd, wv, wg, bias, states, head_gain, wout, gain1, shift1,
    wup, wdown, gain2, shift2,
    out, states_out,
    tok_v, proj_v, out_v, up_v, down_v, state_v, bias_v, hgain_v, gain1_v, shift1_v, gain2_v,
    shift2_v, own_g1, own_s1, bias_t, x_v, a_send, a_recv, a_rows, att_rows, gate_rows, att_recv,
    x_rows, r_own, r_all, normed_v, hidden_v, p_send, p_recv, s_send, s_recv, res_v,
    load_sem, x_ss, x_rs, a_ss, a_rs, t_ss, t_rs, r_ss, r_rs, p_ss, p_rs, s_ss, s_rs, g_ss, g_rs,
    b_ss, b_rs,
):
    members = groups * halves
    my_kv, my_tp = lax.axis_index("kv"), lax.axis_index("tp")
    me = my_kv * halves + my_tp
    rows, cols = tok_v.shape
    width = x_v.shape[1]
    seqs = rows // groups
    heads, kdim = bias_v.shape
    vdim = hgain_v.shape[1]
    kc, vc = kdim // groups, vdim // groups
    nk, nv = heads * kc, heads * vc

    def load(index, src, dst):
        copy = pltpu.make_async_copy(src, dst, load_sem.at[index])
        copy.start()
        return copy

    loads = {}
    loads["tok"] = load(0, tokens, tok_v)
    loads["g1"] = load(1, gain1, own_g1)
    loads["s1"] = load(2, shift1, own_s1)
    loads["bias"] = load(3, bias, bias_v)
    start = 0
    for index, (name, weight) in enumerate((("q", wq), ("k", wk), ("d", wd), ("v", wv), ("g", wg))):
        size = weight.shape[0]
        loads[name] = load(4 + index, weight, proj_v.at[pl.ds(start, size)])
        start += size
    loads["hg"] = load(9, head_gain, hgain_v)
    loads["g2"] = load(10, gain2, gain2_v)
    loads["s2"] = load(11, shift2, shift2_v)
    loads["st"] = load(12, states, state_v)
    loads["out"] = load(13, wout, out_v)
    loads["up"] = load(14, wup, up_v)
    loads["down"] = load(15, wdown, down_v)

    def member(offset):
        index = lax.rem(me + offset, members)
        return index, {"kv": index // halves, "tp": lax.rem(index, halves)}

    def block(index):
        return pl.ds(pl.multiple_of(index * cols, cols), cols)

    barrier = pltpu.get_barrier_semaphore()
    for o in range(1, members):
        pl.semaphore_signal(barrier, inc=1, device_id=member(o)[1], device_id_type=MESH)
    pl.semaphore_wait(barrier, members - 1)

    def remote(src, dst, send, recv, target):
        return pltpu.make_async_remote_copy(
            src_ref=src, dst_ref=dst, send_sem=send, recv_sem=recv, device_id=target,
            device_id_type=MESH,
        )

    def spread(src, place, send, recv):
        copies = []
        for o in range(1, members):
            copy = remote(src, place(me), send.at[o], recv.at[o], member(o)[1])
            copy.start()
            copies.append(copy)
        return copies

    def collect(src, place, send, recv):
        for o in range(1, members):
            source, target = member(members - o)
            remote(src, place(source), send.at[o], recv.at[o], target).wait_recv()

    pending = []
    loads["tok"].wait()
    pending += spread(tok_v, lambda i: x_v.at[:, block(i)], x_ss, x_rs)
    x_v[:, block(me)] = tok_v[...]
    loads["g1"].wait()
    loads["s1"].wait()
    pending += spread(own_g1, lambda i: gain1_v.at[:, block(i)], g_ss, g_rs)
    pending += spread(own_s1, lambda i: shift1_v.at[:, block(i)], b_ss, b_rs)
    gain1_v[:, block(me)] = own_g1[...]
    shift1_v[:, block(me)] = own_s1[...]

    loads["bias"].wait()
    turned = jnp.concatenate([bias_v[...], jnp.zeros((kdim - heads, kdim), F32)], axis=0).T
    lane = lax.broadcasted_iota(jnp.int32, (kc, rows), 1)
    for h in range(heads):
        piece = jnp.zeros((kc, rows), F32)
        for b in range(groups):
            here = (lane >= b * seqs) & (lane < (b + 1) * seqs)
            piece = jnp.where(here, turned[b * kc : (b + 1) * kc, h : h + 1], piece)
        bias_t[h * kc : (h + 1) * kc, :] = piece

    collect(tok_v, lambda i: x_v.at[:, block(i)], x_ss, x_rs)
    x_all = x_v[...]

    def store_projection(first, size):
        got = dot_nt(x_all, proj_v[first : first + size, :]).astype(BF16).astype(F32)
        for a in range(groups):
            a_send[a, :, first : first + size] = got[a * seqs : (a + 1) * seqs, :]

    loads["q"].wait()
    loads["k"].wait()
    store_projection(0, 2 * nk)
    loads["d"].wait()
    store_projection(2 * nk, nk)
    loads["v"].wait()
    store_projection(3 * nk, nv)
    loads["g"].wait()
    store_projection(3 * nk + nv, nv)

    for o in range(1, groups):
        peer = lax.rem(my_kv + o, groups)
        copy = remote(
            a_send.at[peer], a_recv.at[my_kv], a_ss.at[o], a_rs.at[o], {"kv": peer, "tp": my_tp}
        )
        copy.start()
        pending.append(copy)
    a_recv[my_kv] = a_send[my_kv]
    for o in range(1, groups):
        peer = lax.rem(my_kv + groups - o, groups)
        remote(
            a_send.at[peer], a_recv.at[peer], a_ss.at[o], a_rs.at[o], {"kv": peer, "tp": my_tp}
        ).wait_recv()
    for b in range(groups):
        a_rows[b * seqs : (b + 1) * seqs, :] = a_recv[b]

    qt = a_rows[:, 0:nk].T * KEY_DIM ** (-0.5)
    kt = a_rows[:, nk : 2 * nk].T
    zt = a_rows[:, 2 * nk : 3 * nk].T + bias_t[...]
    rt = jnp.exp((jnp.minimum(zt, 0.0) - jnp.log1p(jnp.exp(-jnp.abs(zt)))) / TAU)
    loads["st"].wait()
    for s in range(seqs):
        for h in range(heads):
            first = 3 * nk + h * vc
            values, gates = [], []
            for b in range(groups):
                row = b * seqs + s
                values.append(a_rows[row : row + 1, first : first + vc])
                gates.append(a_rows[row : row + 1, first + nv : first + nv + vc])
            value = jnp.concatenate(values, axis=1)
            gate_rows[s : s + 1, h * vdim : (h + 1) * vdim] = jnp.concatenate(gates, axis=1)
            total = None
            for b in range(groups):
                lanes = slice(b * seqs + s, b * seqs + s + 1)
                subs = slice(h * kc, (h + 1) * kc)
                fresh = (
                    rt[subs, lanes] * state_v[s, h, b * kc : (b + 1) * kc, :]
                    + kt[subs, lanes] * value
                )
                state_v[s, h, b * kc : (b + 1) * kc, :] = fresh
                term = qt[subs, lanes] * fresh
                total = term if total is None else total + term
            att_rows[s : s + 1, h * vdim : (h + 1) * vdim] = jnp.sum(total, axis=0, keepdims=True)
    loads["hg"].wait()
    for h in range(heads):
        span = slice(h * vdim, (h + 1) * vdim)
        readout = att_rows[:, span]
        gate = gate_rows[:, span]
        power = jnp.mean(readout * readout, axis=-1, keepdims=True)
        readout = readout * lax.rsqrt(power + RMS_EPS) * hgain_v[h : h + 1, :]
        att_rows[:, span] = (readout * (gate / (1.0 + jnp.exp(-gate)))).astype(BF16).astype(F32)

    pending += spread(att_rows, lambda i: att_recv.at[i], t_ss, t_rs)
    save = pltpu.make_async_copy(state_v, states_out, load_sem.at[16])
    save.start()
    att_recv[me] = att_rows[...]
    collect(att_rows, lambda i: att_recv.at[i], t_ss, t_rs)
    half = heads * vdim
    for a in range(groups):
        for t in range(halves):
            x_rows[a * seqs : (a + 1) * seqs, t * half : (t + 1) * half] = att_recv[a * halves + t]
    loads["out"].wait()
    mixed = jnp.dot(x_rows[...].astype(BF16), out_v[...], preferred_element_type=F32)
    r_own[...] = ALPHA * tok_v[...].astype(F32) + mixed
    pending += spread(r_own, lambda i: r_all.at[:, block(i)], r_ss, r_rs)
    r_all[:, block(me)] = r_own[...]
    collect(own_g1, lambda i: gain1_v.at[:, block(i)], g_ss, g_rs)
    collect(own_s1, lambda i: shift1_v.at[:, block(i)], b_ss, b_rs)
    collect(r_own, lambda i: r_all.at[:, block(i)], r_ss, r_rs)
    whole = r_all[...]
    average = jnp.sum(whole, axis=-1, keepdims=True) / width
    spread_one = jnp.sum(whole * whole, axis=-1, keepdims=True) / width - average * average
    normed = normalize(whole, average, spread_one, gain1_v[...], shift1_v[...])
    normed_v[...] = normed

    loads["up"].wait()
    units = up_v.shape[1]
    step = min(units, 512)

    def lift(i, carry):
        span = pl.ds(pl.multiple_of(i * step, step), step)
        lifted = jnp.dot(normed_v[...], up_v[:, span], preferred_element_type=F32)
        hidden_v[:, span] = jnp.square(jnp.maximum(lifted, 0.0)).astype(BF16)
        return carry

    lax.fori_loop(0, units // step, lift, 0)
    loads["down"].wait()

    def drop(o, carry):
        index, target = member(o)
        p_send[o] = jnp.dot(hidden_v[...], down_v[:, block(index)], preferred_element_type=F32)
        remote(p_send.at[o], p_recv.at[o], p_ss.at[o], p_rs.at[o], target).start()
        return carry

    lax.fori_loop(1, members, drop, 0)
    total = jnp.dot(hidden_v[...], down_v[:, block(me)], preferred_element_type=F32)
    total = total + ALPHA * normed_v[:, block(me)].astype(F32)
    for o in range(1, members):
        target = member(members - o)[1]
        remote(p_send.at[o], p_recv.at[o], p_ss.at[o], p_rs.at[o], target).wait_recv()
        total = total + p_recv[o]
    sums = jnp.sum(total, axis=-1, keepdims=True)
    squares = jnp.sum(total * total, axis=-1, keepdims=True)
    lane = lax.broadcasted_iota(jnp.int32, s_send.shape, 1)
    stats = jnp.where(lane == 0, sums, squares)
    s_send[...] = stats
    pending += spread(s_send, lambda i: s_recv.at[i], s_ss, s_rs)
    loads["g2"].wait()
    loads["s2"].wait()
    for o in range(1, members):
        source, target = member(members - o)
        remote(s_send, s_recv.at[source], s_ss.at[o], s_rs.at[o], target).wait_recv()
        stats = stats + s_recv[source]
    average = stats[:, 0:1] / width
    spread_two = stats[:, 1:2] / width - average * average
    res_v[...] = normalize(total, average, spread_two, gain2_v[...], shift2_v[...])
    result = pltpu.make_async_copy(res_v, out, load_sem.at[17])
    result.start()
    for copy in pending:
        copy.wait_send()
    for o in range(1, members):
        remote(p_send.at[o], p_recv.at[o], p_ss.at[o], p_rs.at[o], member(o)[1]).wait_send()
    save.wait()
    result.wait()


def fused(groups, halves, *arrays):
    (tokens, wq, wk, wv, wg, wd, bias, states, head_gain, wout, gain1, shift1, wup, wdown, gain2,
     shift2) = arrays

    def flat(weight):
        return weight.transpose(1, 2, 0).reshape(-1, weight.shape[0])

    def row(vector):
        return vector.reshape(1, -1)

    rows, cols = tokens.shape
    members = groups * halves
    width = wq.shape[0]
    seqs, heads, kdim, vdim = states.shape
    proj = 3 * wq.shape[1] * wq.shape[2] + 2 * wv.shape[1] * wv.shape[2]
    vmem = pltpu.VMEM
    dma = pltpu.SemaphoreType.DMA
    anywhere = pl.BlockSpec(memory_space=pl.ANY)
    scratch = [
        vmem((rows, cols), BF16),
        vmem((proj, width), BF16),
        vmem(wout.shape, BF16),
        vmem(wup.shape, BF16),
        vmem(wdown.shape, BF16),
        vmem(states.shape, F32),
        vmem(bias.shape, F32),
        vmem(head_gain.shape, F32),
        vmem((1, width), F32),
        vmem((1, width), F32),
        vmem((1, cols), F32),
        vmem((1, cols), F32),
        vmem((1, cols), F32),
        vmem((1, cols), F32),
        vmem((heads * kdim // groups, rows), F32),
        vmem((rows, width), BF16),
        vmem((groups, seqs, proj), F32),
        vmem((groups, seqs, proj), F32),
        vmem((rows, proj), F32),
        vmem((seqs, heads * vdim), F32),
        vmem((seqs, heads * vdim), F32),
        vmem((members, seqs, heads * vdim), F32),
        vmem((rows, halves * heads * vdim), F32),
        vmem((rows, cols), F32),
        vmem((rows, width), F32),
        vmem((rows, width), BF16),
        vmem((rows, wup.shape[1]), BF16),
        vmem((members, rows, cols), F32),
        vmem((members, rows, cols), F32),
        vmem((rows, 128), F32),
        vmem((members, rows, 128), F32),
        vmem((rows, cols), BF16),
        dma((18,)),
    ]
    for count in (members, groups, members, members, members, members, members, members):
        scratch += [dma((count,)), dma((count,))]
    return pl.pallas_call(
        functools.partial(layer_kernel, groups, halves),
        out_shape=(
            jax.ShapeDtypeStruct(tokens.shape, BF16),
            jax.ShapeDtypeStruct(states.shape, F32),
        ),
        in_specs=[anywhere] * 16,
        out_specs=(anywhere, anywhere),
        scratch_shapes=scratch,
        compiler_params=pltpu.CompilerParams(
            collective_id=0, has_side_effects=True, vmem_limit_bytes=67043328
        ),
    )(
        tokens, flat(wq), flat(wk), flat(wd), flat(wv), flat(wg), bias, states, head_gain, wout,
        row(gain1), row(shift1), wup, wdown, row(gain2), row(shift2),
    )


def dispatch(groups, halves, *arrays):
    rows, cols = arrays[0].shape
    if rows == 8 and cols % 128 == 0 and rows % groups == 0:
        return fused(groups, halves, *arrays)
    return body(*arrays)


def solution(mesh):
    placed = (
        P("dp", ("kv", "tp")),
        P(None, "tp", "kv"),
        P(None, "tp", "kv"),
        P(None, "tp", "kv"),
        P(None, "tp", "kv"),
        P(None, "tp", "kv"),
        P("tp", None),
        P(("dp", "kv"), "tp", None, None),
        P("tp", None),
        P(None, ("kv", "tp")),
        P(("kv", "tp")),
        P(("kv", "tp")),
        P(None, ("kv", "tp")),
        P(("kv", "tp"), None),
        P(("kv", "tp")),
        P(("kv", "tp")),
    )
    return jax.shard_map(
        functools.partial(dispatch, mesh.shape["kv"], mesh.shape["tp"]),
        mesh=mesh,
        in_specs=placed,
        out_specs=(P("dp", ("kv", "tp")), P(("dp", "kv"), "tp", None, None)),
        check_vma=False,
    )
```
